32 devices in a mesh: grp: 2 (over x), ep: 16 (over z, y, core).
Axes of the slice: x: 2, y: 2, z: 4, core: 2. Of those that a mesh axis runs over, the one named last changes fastest.
Arguments:
- tokens: bfloat16 [256, 2048], P(('grp', 'ep')), parts along dimension 0, may hold values from -6 to 6
- first_gain: bfloat16 [2048], replicated, may hold values from 0.099609375 to 1.8984375
- query_weight: bfloat16 [2048, 1024], P(None, 'ep'), may hold values from -0.125 to 0.125
- key_weight: bfloat16 [2048, 1024], P(None, 'ep'), may hold values from -0.125 to 0.125
- value_weight: bfloat16 [2048, 1024], P(None, 'ep'), may hold values from -0.125 to 0.125
- outgate_weight: bfloat16 [2048, 1024], P(None, 'ep'), may hold values from -0.125 to 0.125
- igate_weight: bfloat16 [2048, 8], replicated, may hold values from -0.125 to 0.125
- fgate_weight: bfloat16 [2048, 8], replicated, may hold values from -0.125 to 0.125
- igate_bias: float32 [8], replicated, may hold values from -2 to 1
- fgate_bias: float32 [8], replicated, may hold values from -1 to 4
- memory_state: float32 [256, 8, 128, 128], P(('grp', 'ep')), parts along dimension 0, may hold values from -0.6 to 0.6
- norm_state: float32 [256, 8, 128], P(('grp', 'ep')), parts along dimension 0, may hold values from -0.6 to 0.6
- max_state: float32 [256, 8], P(('grp', 'ep')), parts along dimension 0, may hold values from -1 to 2
- head_gain: bfloat16 [1024], replicated, may hold values from 0.099609375 to 1.8984375
- out_weight: bfloat16 [1024, 2048], P('ep'), may hold values from -0.1875 to 0.1875
- second_gain: bfloat16 [2048], replicated, may hold values from 0.099609375 to 1.8984375
- expert_ids: int32 [256, 6], P(('grp', 'ep')), parts along dimension 0, may hold values from 0 to 15, all different within a row; in each aligned block of 8 rows (0 to 7, 8 to 15, ...) at most 6 rows name the same one
- route_weight: float32 [256, 6], P(('grp', 'ep')), parts along dimension 0, may hold values from 0.2 to 1
- expert_gate: bfloat16 [16, 2048, 256], P('ep'), may hold values from -0.125 to 0.125
- expert_up: bfloat16 [16, 2048, 256], P('ep'), may hold values from -0.125 to 0.125
- expert_down: bfloat16 [16, 256, 2048], P('ep'), may hold values from -0.375 to 0.375
- shared_gate: bfloat16 [2048, 256], P('ep'), may hold values from -0.125 to 0.125
- shared_up: bfloat16 [2048, 256], P('ep'), may hold values from -0.125 to 0.125
- shared_down: bfloat16 [256, 2048], P(None, 'ep'), may hold values from -0.375 to 0.375
Outputs:
- mixed_out: bfloat16 [256, 2048], P(('grp', 'ep')), parts along dimension 0
- memory_next: float32 [256, 8, 128, 128], P(('grp', 'ep')), parts along dimension 0
- norm_next: float32 [256, 8, 128], P(('grp', 'ep')), parts along dimension 0
- max_next: float32 [256, 8], P(('grp', 'ep')), parts along dimension 0
The draws below stay inside these ranges and needn't reach their ends.
There are 2 independent parts, one for each index of `grp`. The reference program is written for one: setup_inputs(seed, part) draws one part's arguments, and reference() takes and returns one part's arrays. A program takes and returns all parts, laid end to end along the dimension named above; an argument that names none is the same for every part. Nothing has to cross between parts.
Inputs may be any that keep to these rules, and one draw needn't show every extreme that they name: `expert_ids`: each row names 6 different experts. Among the rows of one device no expert is named by more than 6 rows, and in every draw some expert is named by exactly 6 rows of some device.
All inputs are finite; a program needn't handle non-finite values.
Results may differ from the reference program's by a relative error of at most 0.013.
Values may be sent and summed in bfloat16 or wider, within the bound.
A program may use at most 64 MiB of HBM per device.

```python
import math
import jax
import jax.numpy as jnp
import numpy as np
from jax import lax

D = 2048
HEADS = 8
DK = 128
FE = 256
FS = 256
TOP_K = 6
SEQ_DEV = 8
MW = 1024
SEQS = 128
EXPERTS = 16
CAP = 6
N_EP = 16


def levels(own_key, shape, pieces, low, high):
    loudness, own = 1.0, jax.random.fold_in(own_key, 6)
    for axis_at, parts in pieces:
        draws = jnp.exp(jax.random.uniform(jax.random.fold_in(own, axis_at), (parts,), jnp.float32, low / len(pieces), high / len(pieces)))
        loudness = loudness * jnp.repeat(draws, shape[axis_at] // parts).reshape([-1 if axis == axis_at else 1 for axis in range(len(shape))])
    return loudness


def routed_block(key, own, number, rows, number_of, top, reach, slope):
    sequence = jax.random.permutation(key, number_of)
    crowded, usual = portions_of(number_of, rows * top, reach, slope, True), portions_of(number_of, rows * top, reach, slope, False)
    places = jnp.arange(number_of)

    def named(tallies, turn):
        used = int((tallies > 0).sum())
        fixed = max(1, used // 4)
        shifted = fixed + (places - fixed + turn * (used - fixed)) % max(1, number_of - fixed)
        return jnp.zeros((number_of,), jnp.int32).at[sequence[jnp.where(places < fixed, places, shifted)]].set(jnp.asarray(tallies, jnp.int32))

    tallies = jnp.where(number % 4 == 0, named(crowded, number // 4), named(usual, number - number // 4 - 1))
    mixed = jax.random.permutation(jax.random.fold_in(own, 3), number_of)
    giver, sink = mixed[0:number_of // 2 * 2:2], mixed[1:number_of // 2 * 2:2]
    room = jnp.minimum(tallies[giver] - 1, reach - tallies[sink]) // 2
    room = jnp.where((giver == sequence[0]) | (sink == sequence[0]) | (tallies[sink] == 0), 0, jnp.maximum(room, 0))
    shifted = jax.random.randint(jax.random.fold_in(own, 4), (number_of // 2,), 0, 1 << 20) % (room + 1)
    tallies = tallies.at[giver].add(-shifted).at[sink].add(shifted)
    items = jnp.searchsorted(jnp.cumsum(tallies), jnp.arange(rows * top), side="right").astype(jnp.int32)
    listing = items.reshape(top, rows).T
    listing = listing[jax.random.permutation(jax.random.fold_in(own, 1), rows)]
    turn = jax.random.randint(jax.random.fold_in(own, 2), (rows, 1), 0, top)
    return jnp.take_along_axis(listing, (jnp.arange(top)[None, :] + turn) % top, axis=1)


def portions_of(number_of, total, limit, slope, full):
    portions = [(1 << 20) // math.isqrt(rank ** slope) + 1 for rank in range(1, number_of + 1)]
    largest = limit if full else min(limit, max(-(-total // number_of), total * portions[0] // sum(portions)))
    least = 1 if total - largest >= number_of - 1 else 0
    given, rest = [largest] + [least] * (number_of - 1), total - largest - least * (number_of - 1)
    while rest > 0:
        candidates = [i for i in range(1, number_of) if given[i] < largest] or [i for i in range(1, number_of) if given[i] < limit]
        mass, budget = sum([portions[i] for i in candidates]), rest
        for i in candidates:
            addition = min(limit - given[i], max(1, budget * portions[i] // mass), rest)
            given[i] = given[i] + addition
            rest = rest - addition
    return np.array(given)


def noise(key, shape, spread, limit, split=(), kind=jnp.bfloat16):
    loudness = levels(key, shape, split, -0.22, 0.18) if split else 1.0
    drawn = jax.random.normal(key, shape, jnp.float32) * spread * loudness
    return jnp.minimum(jnp.maximum(drawn, -limit), limit).astype(kind)


def setup_inputs(seed: int = 0, part: int = 0) -> dict:
    arg_keys = jax.random.split(jax.random.key(seed), 25)
    own_keys = jax.random.split(jax.random.fold_in(arg_keys[24], part), 25)
    tokens = noise(own_keys[0], (SEQS, D), 1.0, 6.0, ((0, 16),))
    first_gain = jnp.clip(1.0 + 0.18 * jax.random.normal(arg_keys[1], (D,), jnp.float32), 0.099609375, 1.8984375).astype(jnp.bfloat16)
    query_weight = noise(arg_keys[2], (D, MW), D ** -0.5, 0.125, ((1, 16),))
    key_weight = noise(arg_keys[3], (D, MW), D ** -0.5, 0.125, ((1, 16),))
    value_weight = noise(arg_keys[4], (D, MW), D ** -0.5, 0.125, ((1, 16),))
    outgate_weight = noise(arg_keys[5], (D, MW), D ** -0.5, 0.125, ((1, 16),))
    igate_weight = noise(arg_keys[6], (D, HEADS), D ** -0.5, 0.125)
    fgate_weight = noise(arg_keys[7], (D, HEADS), D ** -0.5, 0.125)
    igate_bias = jnp.clip(jax.random.uniform(arg_keys[8], (HEADS,), jnp.float32, -2.0, 1.0), -2.0, 1.0)
    fgate_bias = jnp.clip(jax.random.uniform(arg_keys[9], (HEADS,), jnp.float32, -1.0, 4.0), -1.0, 4.0)
    memory_state = noise(own_keys[10], (SEQS, HEADS, DK, DK), 0.1, 0.6, ((0, 16),), jnp.float32)
    norm_state = noise(own_keys[11], (SEQS, HEADS, DK), 0.1, 0.6, ((0, 16),), jnp.float32)
    max_state = jnp.clip(-1.0 + 3.0 * jax.random.uniform(own_keys[12], (SEQS, HEADS), jnp.float32) ** levels(own_keys[12], (SEQS, HEADS), ((0, 16),), -0.2, 0.2), -1.0, 2.0)
    head_gain = jnp.clip(1.0 + 0.18 * jax.random.normal(arg_keys[13], (MW,), jnp.float32), 0.099609375, 1.8984375).astype(jnp.bfloat16)
    out_weight = noise(arg_keys[14], (MW, D), MW ** -0.5, 0.1875, ((0, 16),))
    second_gain = jnp.clip(1.0 + 0.18 * jax.random.normal(arg_keys[15], (D,), jnp.float32), 0.099609375, 1.8984375).astype(jnp.bfloat16)
    expert_ids_keys = jax.random.split(jax.random.fold_in(own_keys[16], 1), SEQS // SEQ_DEV)
    expert_ids_turns = jax.random.permutation(jax.random.fold_in(own_keys[16], 3), SEQS // SEQ_DEV)
    expert_ids = jax.vmap(lambda own, number: routed_block(jax.random.fold_in(own_keys[16], 2), own, number, SEQ_DEV, EXPERTS, TOP_K, CAP, 1))(expert_ids_keys, expert_ids_turns).reshape((SEQS, TOP_K))
    route_weight = jnp.clip(0.2 + 0.8 * jax.random.uniform(own_keys[17], (SEQS, TOP_K), jnp.float32) ** levels(own_keys[17], (SEQS, TOP_K), ((0, 16),), -0.2, 0.2), 0.2, 1.0)
    expert_gate = noise(arg_keys[18], (EXPERTS, D, FE), D ** -0.5, 0.125, ((0, 16),))
    expert_up = noise(arg_keys[19], (EXPERTS, D, FE), D ** -0.5, 0.125, ((0, 16),))
    expert_down = noise(arg_keys[20], (EXPERTS, FE, D), FE ** -0.5, 0.375, ((0, 16),))
    shared_gate = noise(arg_keys[21], (D, FS), D ** -0.5, 0.125, ((0, 16),))
    shared_up = noise(arg_keys[22], (D, FS), D ** -0.5, 0.125, ((0, 16),))
    shared_down = noise(arg_keys[23], (FS, D), FS ** -0.5, 0.375, ((1, 16),))
    return dict(tokens=tokens, first_gain=first_gain, query_weight=query_weight, key_weight=key_weight, value_weight=value_weight, outgate_weight=outgate_weight, igate_weight=igate_weight, fgate_weight=fgate_weight, igate_bias=igate_bias, fgate_bias=fgate_bias, memory_state=memory_state, norm_state=norm_state, max_state=max_state, head_gain=head_gain, out_weight=out_weight, second_gain=second_gain, expert_ids=expert_ids, route_weight=route_weight, expert_gate=expert_gate, expert_up=expert_up, expert_down=expert_down, shared_gate=shared_gate, shared_up=shared_up, shared_down=shared_down)


epsilon = 1e-06

def rms_scale(values, gain):
    return values * lax.rsqrt(lax.optimization_barrier(jnp.mean(values * values, axis=-1, keepdims=True)) + epsilon) * gain.astype(jnp.float32)

def cell_step(normed, query, key_proj, value_proj, outgate, igate_weight, fgate_weight, igate_bias, fgate_bias, memory_state, norm_state, max_state, head_gain):
    row_count, head_count = max_state.shape
    head_size = memory_state.shape[-1]
    input_gate = jnp.dot(normed, igate_weight, preferred_element_type=jnp.float32) + igate_bias
    forget_log = jax.nn.log_sigmoid(jnp.dot(normed, fgate_weight, preferred_element_type=jnp.float32) + fgate_bias)
    query_heads = query.astype(jnp.float32).reshape(row_count, head_count, head_size)
    key_heads = key_proj.astype(jnp.float32).reshape(row_count, head_count, head_size) * head_size ** (-0.5)
    value_heads = value_proj.astype(jnp.float32).reshape(row_count, head_count, head_size)
    max_next = jnp.maximum(forget_log + max_state, input_gate)
    decay_rate = jnp.exp(forget_log + max_state - max_next)
    injected = jnp.exp(input_gate - max_next)
    memory_next = decay_rate[:, :, None, None] * memory_state + injected[:, :, None, None] * (key_heads[:, :, :, None] * value_heads[:, :, None, :])
    norm_next = decay_rate[:, :, None] * norm_state + injected[:, :, None] * key_heads
    numerator = jnp.einsum('shd,shde->she', query_heads, memory_next, precision=lax.Precision.HIGHEST)
    denominator = jnp.maximum(jnp.abs(lax.optimization_barrier(jnp.sum(query_heads * norm_next, axis=-1))), jnp.exp(-max_next))
    readout = numerator / denominator[:, :, None]
    readout = rms_scale(readout, head_gain.reshape(head_count, head_size))
    gated = readout.reshape(row_count, head_count * head_size) * jax.nn.sigmoid(outgate.astype(jnp.float32))
    return (gated.astype(jnp.bfloat16), memory_next, norm_next, max_next)

def expert_apply(picked_rows, gate_matrix, up_matrix, down_matrix):
    gate_sums = jnp.dot(picked_rows, gate_matrix, preferred_element_type=jnp.float32)
    up_sums = jnp.dot(picked_rows, up_matrix, preferred_element_type=jnp.float32)
    hidden = (jax.nn.silu(gate_sums) * up_sums).astype(jnp.bfloat16)
    return jnp.dot(hidden, down_matrix, preferred_element_type=jnp.float32).astype(jnp.bfloat16)

def reference(tokens, first_gain, query_weight, key_weight, value_weight, outgate_weight, igate_weight, fgate_weight, igate_bias, fgate_bias, memory_state, norm_state, max_state, head_gain, out_weight, second_gain, expert_ids, route_weight, expert_gate, expert_up, expert_down, shared_gate, shared_up, shared_down):
    inputs = tokens.astype(jnp.float32)
    normed = rms_scale(inputs, first_gain).astype(jnp.bfloat16)
    query = jnp.dot(normed, query_weight, preferred_element_type=jnp.float32).astype(jnp.bfloat16)
    key_proj = jnp.dot(normed, key_weight, preferred_element_type=jnp.float32).astype(jnp.bfloat16)
    value_proj = jnp.dot(normed, value_weight, preferred_element_type=jnp.float32).astype(jnp.bfloat16)
    outgate = jnp.dot(normed, outgate_weight, preferred_element_type=jnp.float32).astype(jnp.bfloat16)
    gated, memory_next, norm_next, max_next = cell_step(normed, query, key_proj, value_proj, outgate, igate_weight, fgate_weight, igate_bias, fgate_bias, memory_state, norm_state, max_state, head_gain)
    mix = jnp.dot(gated, out_weight, preferred_element_type=jnp.float32).astype(jnp.bfloat16)
    stream = inputs + mix.astype(jnp.float32)
    normed_two = rms_scale(stream, second_gain).astype(jnp.bfloat16)
    padded = jnp.concatenate([normed_two, jnp.zeros((1, D), normed_two.dtype)], axis=0)

    def per_expert(routed, inputs_expert):
        expert_index, gate_matrix, up_matrix, down_matrix = inputs_expert
        chosen = expert_ids == expert_index
        weight = lax.optimization_barrier(jnp.sum(jnp.where(chosen, route_weight, jnp.zeros_like(route_weight)), axis=1))
        weight_pad = jnp.concatenate([weight, jnp.zeros((1,), weight.dtype)], axis=0)
        picked = jnp.nonzero(jnp.any(chosen, axis=1), size=N_EP * CAP, fill_value=SEQS)[0].astype(jnp.int32)
        result = expert_apply(padded[picked], gate_matrix, up_matrix, down_matrix)
        routed = routed.at[picked].add(weight_pad[picked][:, None] * result.astype(routed.dtype), mode='drop')
        return (routed, None)
    routed, _ = lax.scan(per_expert, jnp.zeros((SEQS, D), jnp.float32), (jnp.arange(EXPERTS, dtype=jnp.int32), expert_gate, expert_up, expert_down))
    gate_shared = jnp.dot(normed_two, shared_gate, preferred_element_type=jnp.float32)
    up_shared = jnp.dot(normed_two, shared_up, preferred_element_type=jnp.float32)
    hidden_shared = (jax.nn.silu(gate_shared) * up_shared).astype(jnp.bfloat16)
    shared_result = jnp.dot(hidden_shared, shared_down, preferred_element_type=jnp.float32)
    mixed_out = (stream + routed + shared_result).astype(jnp.bfloat16)
    return (mixed_out, memory_next, norm_next, max_next)
```

```python
import jax
import jax.numpy as jnp
from jax import lax
from jax.experimental import pallas as pl
from jax.experimental.pallas import tpu as pltpu
from jax.sharding import PartitionSpec as P
import functools

epsilon = 1e-06


def rms_scale(values, gain):
    return (
        values
        * lax.rsqrt(jnp.mean(values * values, axis=-1, keepdims=True) + epsilon)
        * gain.astype(jnp.float32)
    )


def cell_step(
    normed,
    query,
    key_proj,
    value_proj,
    outgate,
    igate_weight,
    fgate_weight,
    igate_bias,
    fgate_bias,
    memory_state,
    norm_state,
    max_state,
    head_gain,
):
    row_count, head_count = max_state.shape
    head_size = memory_state.shape[-1]
    input_gate = jnp.dot(normed, igate_weight, preferred_element_type=jnp.float32) + igate_bias
    forget_log = jax.nn.log_sigmoid(
        jnp.dot(normed, fgate_weight, preferred_element_type=jnp.float32) + fgate_bias
    )
    query_heads = query.astype(jnp.float32).reshape(row_count, head_count, head_size)
    key_heads = key_proj.astype(jnp.float32).reshape(
        row_count, head_count, head_size
    ) * head_size ** (-0.5)
    value_heads = value_proj.astype(jnp.float32).reshape(row_count, head_count, head_size)
    max_next = jnp.maximum(forget_log + max_state, input_gate)
    decay_rate = jnp.exp(forget_log + max_state - max_next)
    injected = jnp.exp(input_gate - max_next)
    memory_next = decay_rate[:, :, None, None] * memory_state + injected[:, :, None, None] * (
        key_heads[:, :, :, None] * value_heads[:, :, None, :]
    )
    norm_next = decay_rate[:, :, None] * norm_state + injected[:, :, None] * key_heads
    numerator = jnp.einsum(
        "shd,shde->she", query_heads, memory_next, precision=lax.Precision.HIGHEST
    )
    denominator = jnp.maximum(
        jnp.abs(jnp.sum(query_heads * norm_next, axis=-1)), jnp.exp(-max_next)
    )
    readout = numerator / denominator[:, :, None]
    readout = rms_scale(readout, head_gain.reshape(head_count, head_size))
    gated = readout.reshape(row_count, head_count * head_size) * jax.nn.sigmoid(
        outgate.astype(jnp.float32)
    )
    return (gated.astype(jnp.bfloat16), memory_next, norm_next, max_next)


def shards(
    tokens,
    first_gain,
    query_weight,
    key_weight,
    value_weight,
    outgate_weight,
    igate_weight,
    fgate_weight,
    igate_bias,
    fgate_bias,
    memory_state,
    norm_state,
    max_state,
    head_gain,
    out_weight,
    second_gain,
    expert_ids,
    route_weight,
    expert_gate,
    expert_up,
    expert_down,
    shared_gate,
    shared_up,
    shared_down,
):
    own_rows = tokens.shape[0]
    devices = lax.axis_size("ep")
    top_count = expert_ids.shape[1]
    capacity = max(2, 2 * own_rows * top_count // devices)
    inputs = tokens.astype(jnp.float32)
    normed = rms_scale(inputs, first_gain).astype(jnp.bfloat16)
    block_rows = lax.all_gather(normed, "ep", axis=0, tiled=True)
    columns = jnp.stack(
        [
            jnp.dot(block_rows, matrix, preferred_element_type=jnp.float32).astype(jnp.bfloat16)
            for matrix in (query_weight, key_weight, value_weight, outgate_weight)
        ]
    )
    projected = lax.all_to_all(columns, "ep", split_axis=1, concat_axis=2, tiled=True)
    gated, memory_next, norm_next, max_next = cell_step(
        normed,
        projected[0],
        projected[1],
        projected[2],
        projected[3],
        igate_weight,
        fgate_weight,
        igate_bias,
        fgate_bias,
        memory_state,
        norm_state,
        max_state,
        head_gain,
    )
    picked = gated
    mix_sums = jnp.dot(
        picked,
        lax.all_gather(out_weight, "ep", axis=0, tiled=True),
        preferred_element_type=jnp.float32,
    )
    stream = inputs + mix_sums.astype(jnp.bfloat16).astype(jnp.float32)
    normed_two = rms_scale(stream, second_gain).astype(jnp.bfloat16)
    block_rows = (
        lax.all_gather(shared_gate, "ep", axis=0, tiled=True),
        lax.all_gather(shared_up, "ep", axis=0, tiled=True),
    )
    picked = normed_two
    gate_shared = jnp.dot(picked, block_rows[0], preferred_element_type=jnp.float32)
    up_shared = jnp.dot(picked, block_rows[1], preferred_element_type=jnp.float32)
    hidden_shared = (jax.nn.silu(gate_shared) * up_shared).astype(jnp.bfloat16)
    shared_result = jnp.dot(
        hidden_shared,
        lax.all_gather(shared_down, "ep", axis=1, tiled=True),
        preferred_element_type=jnp.float32,
    )
    choose = (expert_ids[:, :, None] == jnp.arange(devices, dtype=jnp.int32)[None, None, :]).astype(
        jnp.int32
    )
    counted = jnp.sum(choose, axis=1)
    ranking = jnp.cumsum(counted, axis=0) - counted
    slot_index = jnp.sum(choose * ranking[:, None, :], axis=2)
    slot_ids = jnp.arange(capacity, dtype=jnp.int32)
    selector = counted.T[:, None, :] * (ranking.T[:, None, :] == slot_ids[None, :, None]).astype(
        jnp.int32
    )
    outgoing = jnp.einsum(
        "ecr,rd->ecd", selector.astype(jnp.bfloat16), normed_two, preferred_element_type=jnp.float32
    ).astype(jnp.bfloat16)
    arrived = lax.all_to_all(outgoing, "ep", split_axis=0, concat_axis=0, tiled=True)
    sources, slots, width = arrived.shape
    flat_rows = arrived.reshape(sources * slots, width)
    gate_sums = jnp.dot(flat_rows, expert_gate[0], preferred_element_type=jnp.float32)
    up_sums = jnp.dot(flat_rows, expert_up[0], preferred_element_type=jnp.float32)
    hidden = (jax.nn.silu(gate_sums) * up_sums).astype(jnp.bfloat16)
    result = jnp.dot(hidden, expert_down[0], preferred_element_type=jnp.float32).astype(
        jnp.bfloat16
    )
    results = lax.all_to_all(
        result.reshape(sources, slots, width), "ep", split_axis=0, concat_axis=0, tiled=True
    )
    flat_results = results.reshape(devices * capacity, results.shape[2])
    picked_results = flat_results[expert_ids * capacity + slot_index]
    routed = jnp.sum(route_weight[:, :, None] * picked_results.astype(jnp.float32), axis=1)
    mixed_out = (stream + routed + shared_result).astype(jnp.bfloat16)
    return (mixed_out, memory_next, norm_next, max_next)


ANY, VMEM = pl.ANY, pltpu.VMEM
F32, BF16 = jnp.float32, jnp.bfloat16


def remote(source, target, send, receive, device):
    return pltpu.make_async_remote_copy(
        src_ref=source,
        dst_ref=target,
        send_sem=send,
        recv_sem=receive,
        device_id={"ep": device},
        device_id_type=pl.DeviceIdType.MESH,
    )


def fused(
    n,
    tokens,
    first_gain,
    query_weight,
    key_weight,
    value_weight,
    outgate_weight,
    igate_weight,
    fgate_weight,
    igate_bias,
    fgate_bias,
    memory_state,
    norm_state,
    max_state,
    head_gain,
    out_weight,
    second_gain,
    expert_ids,
    route_weight,
    expert_gate,
    expert_up,
    expert_down,
    shared_gate,
    shared_up,
    shared_down,
    mixed_out,
    memory_next,
    norm_next,
    max_next,
    proj_in,
    proj,
    gates_in,
    memory,
    out_pad,
    wide,
    down,
    rows_one,
    rows_two,
    table,
    column_send,
    column_recv,
    shared_send,
    shared_recv,
    sdown_recv,
    gated_send,
    gated_recv,
    part,
    part_send,
    pair_recv,
    sum_send,
    sum_recv,
    local_sem,
    memory_in_sem,
    memory_out_sem,
    send_sem,
    recv_sem,
    gather_sem,
    pair_sem,
    sum_sem,
):
    rows, width = tokens.shape
    heads, size = memory_state.shape[1], memory_state.shape[3]
    cut = query_weight.shape[1]
    share = size // cut
    hidden = shared_gate.shape[1] // n
    top_count = expert_ids.shape[1]
    chips = n // 2
    me = lax.axis_index("ep")
    side, chip = me % 2, me // 2
    partner = me + 1 - 2 * side

    barrier = pltpu.get_barrier_semaphore()
    for k in range(1, n):
        pl.semaphore_signal(
            barrier,
            inc=1,
            device_id={"ep": (me + k) % n},
            device_id_type=pl.DeviceIdType.MESH,
        )

    loads = []

    def load(source, target):
        copy = pltpu.make_async_copy(source, target, local_sem.at[len(loads)])
        copy.start()
        loads.append(copy)
        return copy

    proj_loads = [
        load(matrix, proj_in.at[i])
        for i, matrix in enumerate((query_weight, key_weight, value_weight, outgate_weight))
    ]
    gate_loads = [load(igate_weight, gates_in.at[0]), load(fgate_weight, gates_in.at[1])]
    memory_loads = []
    for h in range(heads):
        copy = pltpu.make_async_copy(
            memory_state.at[:, h], memory.at[:, h], memory_in_sem.at[h]
        )
        copy.start()
        memory_loads.append(copy)
    spot = pl.multiple_of((me % share) * cut, cut)
    out_load = load(out_weight, out_pad.at[pl.ds(spot, cut)])
    wide_loads = [load(expert_gate.at[0], wide.at[0]), load(expert_up.at[0], wide.at[1])]
    down_load = load(expert_down.at[0], down)

    inputs = tokens[...].astype(F32)
    rows_one[me] = rms_scale(inputs, first_gain[...]).astype(BF16)

    pl.semaphore_wait(barrier, n - 1)

    def gather(buffer, which):
        sends = []
        for k in range(chips - 1, 0, -1):
            there = 2 * ((chip + k) % chips) + side
            sends.append(
                remote(
                    buffer.at[me],
                    buffer.at[me],
                    gather_sem.at[which, 0, k],
                    gather_sem.at[which, 1, k],
                    there,
                )
            )
            sends[-1].start()
        near = remote(
            buffer.at[me],
            buffer.at[me],
            gather_sem.at[which, 2, 0],
            gather_sem.at[which, 3, 0],
            partner,
        )
        near.start()
        return sends, near

    def gather_end(buffer, which, sends, near):
        passed = [near]
        for k in ORDER(chips):
            slot = 2 * ((chip + chips - k) % chips) + side
            sends[chips - 1 - k].wait_recv()
            onward = remote(
                buffer.at[slot],
                buffer.at[slot],
                gather_sem.at[which, 2, k],
                gather_sem.at[which, 3, k],
                partner,
            )
            onward.start()
            passed.append(onward)
        for copy in passed:
            copy.wait_recv()
        return sends + passed

    unsent = []
    first = gather(rows_one, 0)

    for copy in proj_loads:
        copy.wait()
    for i in range(4):
        proj[:, i * cut : (i + 1) * cut] = proj_in[i]
    for i in range(1, share):
        other = pl.multiple_of(((me + i) % share) * cut, cut)
        out_pad[pl.ds(other, cut), :] = jnp.zeros((cut, width), BF16)
    lanes = lax.broadcasted_iota(jnp.int32, (rows, 128), 1)
    routes = jnp.zeros((rows, 128), F32)
    for t in range(top_count):
        routes = routes + jnp.where(
            expert_ids[:, t : t + 1] == lanes, route_weight[:, t : t + 1], 0.0
        )
    table[me] = routes
    for i, matrix in enumerate((shared_gate, shared_up)):
        turned = matrix[...].astype(F32).T.reshape(n, hidden, matrix.shape[0])
        shared_send[:, i * hidden : (i + 1) * hidden, :] = turned.astype(BF16)
    for copy in gate_loads:
        copy.wait()
    own = rows_one[me]
    input_gate = jnp.dot(own, gates_in[0], preferred_element_type=F32) + igate_bias[...]
    forget_log = jax.nn.log_sigmoid(
        jnp.dot(own, gates_in[1], preferred_element_type=F32) + fgate_bias[...]
    )
    kept = forget_log + max_state[...]
    top = jnp.maximum(kept, input_gate)
    max_next[...] = top
    decay_rate = jnp.exp(kept - top)
    injected = jnp.exp(input_gate - top)
    floor = jnp.exp(-top)

    unsent += gather_end(rows_one, 0, *first)

    def flat(buffer):
        held = buffer[...].astype(F32)
        return held.reshape(n * rows, held.shape[2])

    columns = jnp.dot(flat(rows_one).astype(BF16), proj[...], preferred_element_type=F32)
    column_send[...] = columns.reshape(n, rows, 4 * cut).astype(BF16)

    def spread(which, source, target):
        for k in range(1, n):
            there = (me + k) % n
            copy = remote(
                source(there), target, send_sem.at[which, k], recv_sem.at[which, k], there
            )
            copy.start()
            unsent.append(copy)

    def arrive(which, source, target):
        for k in range(1, n):
            remote(
                source(me), target, send_sem.at[which, k], recv_sem.at[which, k], (me + k) % n
            ).wait_recv()

    spread(0, lambda j: column_send.at[j], column_recv.at[me])
    column_recv[me] = column_send[me]
    spread(1, lambda j: table.at[me], table.at[me])
    arrive(0, lambda j: column_send.at[j], column_recv.at[me])
    spread(2, lambda j: shared_send.at[j], shared_recv.at[me])
    shared_recv[me] = shared_send[me]
    spread(3, lambda j: shared_down.at[j], sdown_recv.at[me])
    sdown_recv[me] = shared_down[me]

    memory_stores = []
    for h in range(heads):
        pieces = [column_recv[h * share + i].astype(F32) for i in range(share)]
        query, keyed, valued, outgate = [
            jnp.concatenate([piece[:, i * cut : (i + 1) * cut] for piece in pieces], axis=1)
            for i in range(4)
        ]
        decay = jnp.broadcast_to(decay_rate[:, h : h + 1], (rows, size))
        inject = keyed * size ** (-0.5) * injected[:, h : h + 1]
        norm = decay * norm_state[:, h, :] + inject
        norm_next[:, h, :] = norm
        bottom = jnp.maximum(
            jnp.abs(jnp.sum(query * norm, axis=-1, keepdims=True)), floor[:, h : h + 1]
        )
        key_columns, query_columns = inject.T, query.T
        memory_loads[h].wait()
        tops = []
        for s in range(rows):
            cell = (
                decay[s : s + 1, :] * memory[s, h]
                + key_columns[:, s : s + 1] * valued[s : s + 1, :]
            )
            memory[s, h] = cell
            tops.append(jnp.sum(query_columns[:, s : s + 1] * cell, axis=0, keepdims=True))
        store = pltpu.make_async_copy(
            memory.at[:, h], memory_next.at[:, h], memory_out_sem.at[h]
        )
        store.start()
        memory_stores.append(store)
        readout = jnp.concatenate(tops, axis=0) / bottom
        readout = rms_scale(readout, head_gain[h : h + 1, :])
        gated_send[h] = (readout * jax.nn.sigmoid(outgate)).astype(BF16)

    spread(4, lambda j: gated_send.at[j // share], gated_recv.at[me])
    gated_recv[me] = gated_send[me // share]
    out_load.wait()
    arrive(4, lambda j: gated_send.at[j // share], gated_recv.at[me])

    def scatter(which, total, value):
        part[...] = value.reshape(n, rows, width)
        pair = []
        for k in list(range(1, chips)) + [0]:
            c = (chip + k) % chips
            part_send[which, c] = part[2 * c + 1 - side].astype(BF16)
            copy = remote(
                part_send.at[which, c],
                pair_recv.at[which, c],
                pair_sem.at[which, 0, k],
                pair_sem.at[which, 1, k],
                partner,
            )
            copy.start()
            pair.append((k, c, copy))
        sends = []
        for k, c, copy in pair:
            copy.wait_recv()
            both = part[2 * c + side] + pair_recv[which, c].astype(F32)
            if k == 0:
                total = total + both if total is not None else both
                continue
            sum_send[which, c] = both.astype(BF16)
            away = remote(
                sum_send.at[which, c],
                sum_recv.at[which, chip],
                sum_sem.at[which, 0, k],
                sum_sem.at[which, 1, k],
                2 * c + side,
            )
            away.start()
            sends.append((k, away))
        for k, away in sends:
            away.wait_recv()
            total = total + sum_recv[which, (chip + chips - k) % chips].astype(F32)
        unsent.extend([copy for _, _, copy in pair] + [away for _, away in sends])
        return total

    mix = scatter(
        0, None, jnp.dot(flat(gated_recv).astype(BF16), out_pad[...], preferred_element_type=F32)
    )
    stream = tokens[...].astype(F32) + mix.astype(BF16).astype(F32)
    rows_two[me] = rms_scale(stream, second_gain[...]).astype(BF16)
    second = gather(rows_two, 1)
    for copy in wide_loads + [down_load]:
        copy.wait()
    arrive(1, lambda j: table.at[me], table.at[me])
    arrive(2, lambda j: shared_send.at[j], shared_recv.at[me])
    arrive(3, lambda j: shared_down.at[j], sdown_recv.at[me])
    weights = flat(table)
    mine = lax.broadcasted_iota(jnp.int32, weights.shape, 1) == me
    weight = jnp.sum(jnp.where(mine, weights, 0.0), axis=1, keepdims=True)
    shared_wide = jnp.concatenate([shared_recv[i] for i in range(n)], axis=1)
    shared_rows = jnp.concatenate([sdown_recv[i] for i in range(n)], axis=1)
    unsent += gather_end(rows_two, 1, *second)

    block = flat(rows_two).astype(BF16)
    gate_sums = jnp.dot(block, wide[0], preferred_element_type=F32)
    up_sums = jnp.dot(block, wide[1], preferred_element_type=F32)
    own_hidden = (jax.nn.silu(gate_sums) * up_sums).astype(BF16)
    both = lax.dot_general(
        block, shared_wide, (((1,), (1,)), ((), ())), preferred_element_type=F32
    )
    shared_hidden = (jax.nn.silu(both[:, :hidden]) * both[:, hidden:]).astype(BF16)
    value = weight * jnp.dot(own_hidden, down[...], preferred_element_type=F32) + jnp.dot(
        shared_hidden, shared_rows, preferred_element_type=F32
    )
    mixed_out[...] = scatter(1, stream, value).astype(BF16)

    for copy in unsent:
        copy.wait_send()
    for copy in memory_stores:
        copy.wait()


def ORDER(chips):
    return range(chips - 1, 0, -1)


def fused_shards(n, *args):
    (tokens, first_gain, query_weight, key_weight, value_weight, outgate_weight, igate_weight,
     fgate_weight, igate_bias, fgate_bias, memory_state, norm_state, max_state, head_gain,
     out_weight, second_gain, expert_ids, route_weight, expert_gate, expert_up, expert_down,
     shared_gate, shared_up, shared_down) = args
    rows, width = tokens.shape
    heads, size = memory_state.shape[1], memory_state.shape[3]
    cut = query_weight.shape[1]
    hidden = shared_gate.shape[1] // n
    chips = n // 2
    inner = expert_gate.shape[2]
    operands = (
        tokens, first_gain.reshape(1, -1), query_weight, key_weight, value_weight, outgate_weight,
        igate_weight, fgate_weight, igate_bias.reshape(1, -1), fgate_bias.reshape(1, -1),
        memory_state, norm_state, max_state, head_gain.reshape(heads, size), out_weight,
        second_gain.reshape(1, -1), expert_ids, route_weight, expert_gate, expert_up, expert_down,
        shared_gate, shared_up, shared_down.reshape(n, hidden, shared_down.shape[1]),
    )
    far = {2, 3, 4, 5, 6, 7, 10, 14, 18, 19, 20}
    dma = pltpu.SemaphoreType.DMA
    return pl.pallas_call(
        functools.partial(fused, n),
        out_shape=(
            jax.ShapeDtypeStruct((rows, width), BF16),
            jax.ShapeDtypeStruct(memory_state.shape, F32),
            jax.ShapeDtypeStruct(norm_state.shape, F32),
            jax.ShapeDtypeStruct(max_state.shape, F32),
        ),
        in_specs=[
            pl.BlockSpec(memory_space=ANY if i in far else VMEM) for i in range(len(operands))
        ],
        out_specs=tuple(pl.BlockSpec(memory_space=m) for m in (VMEM, ANY, VMEM, VMEM)),
        scratch_shapes=[
            VMEM((4, width, cut), BF16),
            VMEM((width, 4 * cut), BF16),
            VMEM((2, width, heads), BF16),
            VMEM(memory_state.shape, F32),
            VMEM((size, width), BF16),
            VMEM((2, width, inner), BF16),
            VMEM((inner, width), BF16),
            VMEM((n, rows, width), BF16),
            VMEM((n, rows, width), BF16),
            VMEM((n, rows, 128), F32),
            VMEM((n, rows, 4 * cut), BF16),
            VMEM((n, rows, 4 * cut), BF16),
            VMEM((n, 2 * hidden, shared_gate.shape[0]), BF16),
            VMEM((n, 2 * hidden, shared_gate.shape[0]), BF16),
            VMEM((n, hidden, shared_down.shape[1]), BF16),
            VMEM((heads, rows, size), BF16),
            VMEM((n, rows, size), BF16),
            VMEM((n, rows, width), F32),
            VMEM((2, chips, rows, width), BF16),
            VMEM((2, chips, rows, width), BF16),
            VMEM((2, chips, rows, width), BF16),
            VMEM((2, chips, rows, width), BF16),
            dma((10,)),
            dma((heads,)),
            dma((heads,)),
            dma((5, n)),
            dma((5, n)),
            dma((2, 4, chips)),
            dma((2, 2, chips)),
            dma((2, 2, chips)),
        ],
        compiler_params=pltpu.CompilerParams(
            collective_id=0, has_side_effects=True, vmem_limit_bytes=60 * 1024 * 1024
        ),
    )(*operands)


def fits(n, width, size, cut, hidden_all, experts, rows):
    return (
        n % 2 == 0
        and n <= 128
        and experts == n
        and width % (128 * n) == 0
        and hidden_all % (16 * n) == 0
        and size == 128
        and size % cut == 0
        and cut % 16 == 0
        and rows == 8
    )


def pick(n, *args):
    tokens, query_weight, memory_state = args[0], args[2], args[10]
    experts, hidden_all = args[18].shape[0] * n, args[21].shape[1]
    if fits(
        n, tokens.shape[1], memory_state.shape[3], query_weight.shape[1], hidden_all, experts,
        tokens.shape[0],
    ):
        return fused_shards(n, *args)
    return shards(*args)


def solution(mesh):
    placed = (
        P(("grp", "ep"), None),
        P(),
        P(None, "ep"),
        P(None, "ep"),
        P(None, "ep"),
        P(None, "ep"),
        P(),
        P(),
        P(),
        P(),
        P(("grp", "ep"), None, None, None),
        P(("grp", "ep"), None, None),
        P(("grp", "ep"), None),
        P(),
        P("ep", None),
        P(),
        P(("grp", "ep"), None),
        P(("grp", "ep"), None),
        P("ep", None, None),
        P("ep", None, None),
        P("ep", None, None),
        P("ep", None),
        P("ep", None),
        P(None, "ep"),
    )
    return jax.shard_map(
        functools.partial(pick, mesh.shape["ep"]),
        mesh=mesh,
        in_specs=placed,
        out_specs=(
            P(("grp", "ep"), None),
            P(("grp", "ep"), None, None, None),
            P(("grp", "ep"), None, None),
            P(("grp", "ep"), None),
        ),
        check_vma=False,
    )
```

```python
import jax
import jax.numpy as jnp
from jax import lax
from jax.experimental import pallas as pl
from jax.experimental.pallas import tpu as pltpu
from jax.sharding import PartitionSpec as P
import functools

epsilon = 1e-06


def rms_scale(values, gain):
    return (
        values
        * lax.rsqrt(jnp.mean(values * values, axis=-1, keepdims=True) + epsilon)
        * gain.astype(jnp.float32)
    )


def cell_step(
    normed,
    query,
    key_proj,
    value_proj,
    outgate,
    igate_weight,
    fgate_weight,
    igate_bias,
    fgate_bias,
    memory_state,
    norm_state,
    max_state,
    head_gain,
):
    row_count, head_count = max_state.shape
    head_size = memory_state.shape[-1]
    input_gate = jnp.dot(normed, igate_weight, preferred_element_type=jnp.float32) + igate_bias
    forget_log = jax.nn.log_sigmoid(
        jnp.dot(normed, fgate_weight, preferred_element_type=jnp.float32) + fgate_bias
    )
    query_heads = query.astype(jnp.float32).reshape(row_count, head_count, head_size)
    key_heads = key_proj.astype(jnp.float32).reshape(
        row_count, head_count, head_size
    ) * head_size ** (-0.5)
    value_heads = value_proj.astype(jnp.float32).reshape(row_count, head_count, head_size)
    max_next = jnp.maximum(forget_log + max_state, input_gate)
    decay_rate = jnp.exp(forget_log + max_state - max_next)
    injected = jnp.exp(input_gate - max_next)
    memory_next = decay_rate[:, :, None, None] * memory_state + injected[:, :, None, None] * (
        key_heads[:, :, :, None] * value_heads[:, :, None, :]
    )
    norm_next = decay_rate[:, :, None] * norm_state + injected[:, :, None] * key_heads
    numerator = jnp.einsum(
        "shd,shde->she", query_heads, memory_next, precision=lax.Precision.HIGHEST
    )
    denominator = jnp.maximum(
        jnp.abs(jnp.sum(query_heads * norm_next, axis=-1)), jnp.exp(-max_next)
    )
    readout = numerator / denominator[:, :, None]
    readout = rms_scale(readout, head_gain.reshape(head_count, head_size))
    gated = readout.reshape(row_count, head_count * head_size) * jax.nn.sigmoid(
        outgate.astype(jnp.float32)
    )
    return (gated.astype(jnp.bfloat16), memory_next, norm_next, max_next)


def shards(
    tokens,
    first_gain,
    query_weight,
    key_weight,
    value_weight,
    outgate_weight,
    igate_weight,
    fgate_weight,
    igate_bias,
    fgate_bias,
    memory_state,
    norm_state,
    max_state,
    head_gain,
    out_weight,
    second_gain,
    expert_ids,
    route_weight,
    expert_gate,
    expert_up,
    expert_down,
    shared_gate,
    shared_up,
    shared_down,
):
    own_rows = tokens.shape[0]
    devices = lax.axis_size("ep")
    top_count = expert_ids.shape[1]
    capacity = max(2, 2 * own_rows * top_count // devices)
    inputs = tokens.astype(jnp.float32)
    normed = rms_scale(inputs, first_gain).astype(jnp.bfloat16)
    block_rows = lax.all_gather(normed, "ep", axis=0, tiled=True)
    columns = jnp.stack(
        [
            jnp.dot(block_rows, matrix, preferred_element_type=jnp.float32).astype(jnp.bfloat16)
            for matrix in (query_weight, key_weight, value_weight, outgate_weight)
        ]
    )
    projected = lax.all_to_all(columns, "ep", split_axis=1, concat_axis=2, tiled=True)
    gated, memory_next, norm_next, max_next = cell_step(
        normed,
        projected[0],
        projected[1],
        projected[2],
        projected[3],
        igate_weight,
        fgate_weight,
        igate_bias,
        fgate_bias,
        memory_state,
        norm_state,
        max_state,
        head_gain,
    )
    picked = gated
    mix_sums = jnp.dot(
        picked,
        lax.all_gather(out_weight, "ep", axis=0, tiled=True),
        preferred_element_type=jnp.float32,
    )
    stream = inputs + mix_sums.astype(jnp.bfloat16).astype(jnp.float32)
    normed_two = rms_scale(stream, second_gain).astype(jnp.bfloat16)
    block_rows = (
        lax.all_gather(shared_gate, "ep", axis=0, tiled=True),
        lax.all_gather(shared_up, "ep", axis=0, tiled=True),
    )
    picked = normed_two
    gate_shared = jnp.dot(picked, block_rows[0], preferred_element_type=jnp.float32)
    up_shared = jnp.dot(picked, block_rows[1], preferred_element_type=jnp.float32)
    hidden_shared = (jax.nn.silu(gate_shared) * up_shared).astype(jnp.bfloat16)
    shared_result = jnp.dot(
        hidden_shared,
        lax.all_gather(shared_down, "ep", axis=1, tiled=True),
        preferred_element_type=jnp.float32,
    )
    choose = (expert_ids[:, :, None] == jnp.arange(devices, dtype=jnp.int32)[None, None, :]).astype(
        jnp.int32
    )
    counted = jnp.sum(choose, axis=1)
    ranking = jnp.cumsum(counted, axis=0) - counted
    slot_index = jnp.sum(choose * ranking[:, None, :], axis=2)
    slot_ids = jnp.arange(capacity, dtype=jnp.int32)
    selector = counted.T[:, None, :] * (ranking.T[:, None, :] == slot_ids[None, :, None]).astype(
        jnp.int32
    )
    outgoing = jnp.einsum(
        "ecr,rd->ecd", selector.astype(jnp.bfloat16), normed_two, preferred_element_type=jnp.float32
    ).astype(jnp.bfloat16)
    arrived = lax.all_to_all(outgoing, "ep", split_axis=0, concat_axis=0, tiled=True)
    sources, slots, width = arrived.shape
    flat_rows = arrived.reshape(sources * slots, width)
    gate_sums = jnp.dot(flat_rows, expert_gate[0], preferred_element_type=jnp.float32)
    up_sums = jnp.dot(flat_rows, expert_up[0], preferred_element_type=jnp.float32)
    hidden = (jax.nn.silu(gate_sums) * up_sums).astype(jnp.bfloat16)
    result = jnp.dot(hidden, expert_down[0], preferred_element_type=jnp.float32).astype(
        jnp.bfloat16
    )
    results = lax.all_to_all(
        result.reshape(sources, slots, width), "ep", split_axis=0, concat_axis=0, tiled=True
    )
    flat_results = results.reshape(devices * capacity, results.shape[2])
    picked_results = flat_results[expert_ids * capacity + slot_index]
    routed = jnp.sum(route_weight[:, :, None] * picked_results.astype(jnp.float32), axis=1)
    mixed_out = (stream + routed + shared_result).astype(jnp.bfloat16)
    return (mixed_out, memory_next, norm_next, max_next)


ANY, VMEM = pl.ANY, pltpu.VMEM
F32, BF16 = jnp.float32, jnp.bfloat16


def remote(source, target, send, receive, device):
    return pltpu.make_async_remote_copy(
        src_ref=source,
        dst_ref=target,
        send_sem=send,
        recv_sem=receive,
        device_id={"ep": device},
        device_id_type=pl.DeviceIdType.MESH,
    )


def across(left, right):
    return lax.dot_general(left, right, (((1,), (1,)), ((), ())), preferred_element_type=F32)


def in_line(gain):
    held = gain[...].astype(F32)
    return jnp.concatenate([held[i : i + 1] for i in range(held.shape[0])], axis=1)


def fused(
    n,
    tokens,
    first_gain,
    query_weight,
    key_weight,
    value_weight,
    outgate_weight,
    igate_weight,
    fgate_weight,
    igate_bias,
    fgate_bias,
    memory_state,
    norm_state,
    max_state,
    head_gain,
    out_weight,
    second_gain,
    expert_ids,
    route_weight,
    expert_gate,
    expert_up,
    expert_down,
    shared_gate,
    shared_up,
    shared_down,
    mixed_out,
    memory_next,
    norm_next,
    max_next,
    proj,
    gates_in,
    memory,
    out_pad,
    wide,
    down,
    rows_one,
    rows_two,
    table,
    column_send,
    column_recv,
    shared_send,
    shared_recv,
    sdown_recv,
    gated_send,
    gated_recv,
    part,
    part_send,
    pair_recv,
    sum_send,
    sum_recv,
    local_sem,
    memory_in_sem,
    memory_out_sem,
    send_sem,
    recv_sem,
    gather_sem,
    pair_sem,
    sum_sem,
):
    rows, width = tokens.shape
    heads, size = memory_state.shape[1], memory_state.shape[3]
    cut = query_weight.shape[0]
    share = size // cut
    hidden = shared_gate.shape[1] // n
    top_count = expert_ids.shape[1]
    chips = n // 2
    me = lax.axis_index("ep")
    side, chip = me % 2, me // 2
    partner = me + 1 - 2 * side

    barrier = pltpu.get_barrier_semaphore()
    for k in range(1, n):
        pl.semaphore_signal(
            barrier,
            inc=1,
            device_id={"ep": (me + k) % n},
            device_id_type=pl.DeviceIdType.MESH,
        )

    loads = []

    def load(source, target):
        copy = pltpu.make_async_copy(source, target, local_sem.at[len(loads)])
        copy.start()
        loads.append(copy)
        return copy

    proj_loads = [
        load(matrix, proj.at[pl.ds(i * cut, cut)])
        for i, matrix in enumerate((query_weight, key_weight, value_weight, outgate_weight))
    ]
    gate_loads = [load(igate_weight, gates_in.at[0]), load(fgate_weight, gates_in.at[1])]
    memory_loads = []
    for h in range(heads):
        copy = pltpu.make_async_copy(
            memory_state.at[:, h], memory.at[:, h], memory_in_sem.at[h]
        )
        copy.start()
        memory_loads.append(copy)
    spot = pl.multiple_of((me % share) * cut, cut)
    out_load = load(out_weight, out_pad.at[pl.ds(spot, cut)])
    wide_loads = [load(expert_gate.at[0], wide.at[0]), load(expert_up.at[0], wide.at[1])]
    down_load = load(expert_down.at[0], down)

    inputs = tokens[...].astype(F32)
    rows_one[me] = rms_scale(inputs, in_line(first_gain)).astype(BF16)

    pl.semaphore_wait(barrier, n - 1)

    def gather(buffer, which):
        sends = []
        for k in range(chips - 1, 0, -1):
            there = 2 * ((chip + k) % chips) + side
            sends.append(
                remote(
                    buffer.at[me],
                    buffer.at[me],
                    gather_sem.at[which, 0, k],
                    gather_sem.at[which, 1, k],
                    there,
                )
            )
            sends[-1].start()
        near = remote(
            buffer.at[me],
            buffer.at[me],
            gather_sem.at[which, 2, 0],
            gather_sem.at[which, 3, 0],
            partner,
        )
        near.start()
        return sends, near

    def gather_end(buffer, which, sends, near):
        passed = [near]
        for k in ORDER(chips):
            slot = 2 * ((chip + chips - k) % chips) + side
            sends[chips - 1 - k].wait_recv()
            onward = remote(
                buffer.at[slot],
                buffer.at[slot],
                gather_sem.at[which, 2, k],
                gather_sem.at[which, 3, k],
                partner,
            )
            onward.start()
            passed.append(onward)
        for copy in passed:
            copy.wait_recv()
        return sends + passed

    unsent = []
    first = gather(rows_one, 0)

    for i in range(1, share):
        other = pl.multiple_of(((me + i) % share) * cut, cut)
        out_pad[pl.ds(other, cut), :] = jnp.zeros((cut, width), BF16)
    lanes = lax.broadcasted_iota(jnp.int32, (rows, 128), 1)
    routes = jnp.zeros((rows, 128), F32)
    for t in range(top_count):
        routes = routes + jnp.where(
            expert_ids[:, t : t + 1] == lanes, route_weight[:, t : t + 1], 0.0
        )
    table[me] = routes
    for i, matrix in enumerate((shared_gate, shared_up)):
        turned = matrix[...].astype(F32).T.reshape(n, hidden, matrix.shape[0])
        shared_send[:, i * hidden : (i + 1) * hidden, :] = turned.astype(BF16)
    for copy in gate_loads:
        copy.wait()
    own = rows_one[me]
    input_gate = across(own, gates_in[0]) + igate_bias[...]
    forget_log = jax.nn.log_sigmoid(across(own, gates_in[1]) + fgate_bias[...])
    kept = forget_log + max_state[...]
    top = jnp.maximum(kept, input_gate)
    max_next[...] = top
    decay_rate = jnp.exp(kept - top)
    injected = jnp.exp(input_gate - top)
    floor = jnp.exp(-top)

    unsent += gather_end(rows_one, 0, *first)

    def flat(buffer):
        held = buffer[...].astype(F32)
        return held.reshape(n * rows, held.shape[2])

    for copy in proj_loads:
        copy.wait()
    columns = across(flat(rows_one).astype(BF16), proj[...])
    column_send[...] = columns.reshape(n, rows, 4 * cut).astype(BF16)

    def spread(which, source, target):
        for k in range(1, n):
            there = (me + k) % n
            copy = remote(
                source(there), target, send_sem.at[which, k], recv_sem.at[which, k], there
            )
            copy.start()
            unsent.append(copy)

    def arrive(which, source, target):
        for k in range(1, n):
            remote(
                source(me), target, send_sem.at[which, k], recv_sem.at[which, k], (me + k) % n
            ).wait_recv()

    spread(0, lambda j: column_send.at[j], column_recv.at[me])
    column_recv[me] = column_send[me]
    spread(1, lambda j: table.at[me], table.at[me])
    arrive(0, lambda j: column_send.at[j], column_recv.at[me])
    spread(2, lambda j: shared_send.at[j], shared_recv.at[me])
    shared_recv[me] = shared_send[me]
    spread(3, lambda j: shared_down.at[j], sdown_recv.at[me])
    sdown_recv[me] = shared_down[me]

    memory_stores = []
    for h in range(heads):
        pieces = [column_recv[h * share + i].astype(F32) for i in range(share)]
        query, keyed, valued, outgate = [
            jnp.concatenate([piece[:, i * cut : (i + 1) * cut] for piece in pieces], axis=1)
            for i in range(4)
        ]
        decay = jnp.broadcast_to(decay_rate[:, h : h + 1], (rows, size))
        inject = keyed * size ** (-0.5) * injected[:, h : h + 1]
        norm = decay * norm_state[:, h, :] + inject
        norm_next[:, h, :] = norm
        bottom = jnp.maximum(
            jnp.abs(jnp.sum(query * norm, axis=-1, keepdims=True)), floor[:, h : h + 1]
        )
        key_columns, query_columns = inject.T, query.T
        memory_loads[h].wait()
        tops = []
        for s in range(rows):
            cell = (
                decay[s : s + 1, :] * memory[s, h]
                + key_columns[:, s : s + 1] * valued[s : s + 1, :]
            )
            memory[s, h] = cell
            tops.append(jnp.sum(query_columns[:, s : s + 1] * cell, axis=0, keepdims=True))
        store = pltpu.make_async_copy(
            memory.at[:, h], memory_next.at[:, h], memory_out_sem.at[h]
        )
        store.start()
        memory_stores.append(store)
        readout = jnp.concatenate(tops, axis=0) / bottom
        readout = rms_scale(readout, head_gain[h : h + 1, :])
        gated_send[h] = (readout * jax.nn.sigmoid(outgate)).astype(BF16)

    spread(4, lambda j: gated_send.at[j // share], gated_recv.at[me])
    gated_recv[me] = gated_send[me // share]
    out_load.wait()
    arrive(4, lambda j: gated_send.at[j // share], gated_recv.at[me])

    def scatter(which, total, value):
        part[...] = value.reshape(n, rows, width)
        pair = []
        for k in list(range(1, chips)) + [0]:
            c = (chip + k) % chips
            part_send[which, c] = part[2 * c + 1 - side].astype(BF16)
            copy = remote(
                part_send.at[which, c],
                pair_recv.at[which, c],
                pair_sem.at[which, 0, k],
                pair_sem.at[which, 1, k],
                partner,
            )
            copy.start()
            pair.append((k, c, copy))
        sends = []
        for k, c, copy in pair:
            copy.wait_recv()
            both = part[2 * c + side] + pair_recv[which, c].astype(F32)
            if k == 0:
                total = total + both if total is not None else both
                continue
            sum_send[which, c] = both.astype(BF16)
            away = remote(
                sum_send.at[which, c],
                sum_recv.at[which, chip],
                sum_sem.at[which, 0, k],
                sum_sem.at[which, 1, k],
                2 * c + side,
            )
            away.start()
            sends.append((k, away))
        for k, away in sends:
            away.wait_recv()
            total = total + sum_recv[which, (chip + chips - k) % chips].astype(F32)
        unsent.extend([copy for _, _, copy in pair] + [away for _, away in sends])
        return total

    mix = scatter(
        0, None, jnp.dot(flat(gated_recv).astype(BF16), out_pad[...], preferred_element_type=F32)
    )
    stream = tokens[...].astype(F32) + mix.astype(BF16).astype(F32)
    rows_two[me] = rms_scale(stream, in_line(second_gain)).astype(BF16)
    second = gather(rows_two, 1)
    for copy in wide_loads + [down_load]:
        copy.wait()
    arrive(1, lambda j: table.at[me], table.at[me])
    arrive(2, lambda j: shared_send.at[j], shared_recv.at[me])
    arrive(3, lambda j: shared_down.at[j], sdown_recv.at[me])
    weights = flat(table)
    mine = lax.broadcasted_iota(jnp.int32, weights.shape, 1) == me
    weight = jnp.sum(jnp.where(mine, weights, 0.0), axis=1, keepdims=True)
    shared_wide = jnp.concatenate([shared_recv[i] for i in range(n)], axis=1)
    shared_rows = jnp.concatenate([sdown_recv[i] for i in range(n)], axis=1)
    unsent += gather_end(rows_two, 1, *second)

    block = flat(rows_two).astype(BF16)
    gate_sums = jnp.dot(block, wide[0], preferred_element_type=F32)
    up_sums = jnp.dot(block, wide[1], preferred_element_type=F32)
    own_hidden = (jax.nn.silu(gate_sums) * up_sums).astype(BF16)
    both = across(block, shared_wide)
    shared_hidden = (jax.nn.silu(both[:, :hidden]) * both[:, hidden:]).astype(BF16)
    value = weight * jnp.dot(own_hidden, down[...], preferred_element_type=F32) + jnp.dot(
        shared_hidden, shared_rows, preferred_element_type=F32
    )
    mixed_out[...] = scatter(1, stream, value).astype(BF16)

    for copy in unsent:
        copy.wait_send()
    for copy in memory_stores:
        copy.wait()


def ORDER(chips):
    return range(chips - 1, 0, -1)


def fused_shards(n, *args):
    (tokens, first_gain, query_weight, key_weight, value_weight, outgate_weight, igate_weight,
     fgate_weight, igate_bias, fgate_bias, memory_state, norm_state, max_state, head_gain,
     out_weight, second_gain, expert_ids, route_weight, expert_gate, expert_up, expert_down,
     shared_gate, shared_up, shared_down) = args
    rows, width = tokens.shape
    heads, size = memory_state.shape[1], memory_state.shape[3]
    cut = query_weight.shape[1]
    hidden = shared_gate.shape[1] // n
    chips = n // 2
    inner = expert_gate.shape[2]
    operands = (
        tokens, first_gain.reshape(-1, 128), query_weight.T, key_weight.T, value_weight.T,
        outgate_weight.T, igate_weight.T, fgate_weight.T, igate_bias.reshape(1, -1), fgate_bias.reshape(1, -1),
        memory_state, norm_state, max_state, head_gain.reshape(heads, size), out_weight,
        second_gain.reshape(-1, 128), expert_ids, route_weight, expert_gate, expert_up, expert_down,
        shared_gate, shared_up, shared_down.reshape(n, hidden, shared_down.shape[1]),
    )
    far = {2, 3, 4, 5, 6, 7, 10, 14, 18, 19, 20}
    dma = pltpu.SemaphoreType.DMA
    return pl.pallas_call(
        functools.partial(fused, n),
        out_shape=(
            jax.ShapeDtypeStruct((rows, width), BF16),
            jax.ShapeDtypeStruct(memory_state.shape, F32),
            jax.ShapeDtypeStruct(norm_state.shape, F32),
            jax.ShapeDtypeStruct(max_state.shape, F32),
        ),
        in_specs=[
            pl.BlockSpec(memory_space=ANY if i in far else VMEM) for i in range(len(operands))
        ],
        out_specs=tuple(pl.BlockSpec(memory_space=m) for m in (VMEM, ANY, VMEM, VMEM)),
        scratch_shapes=[
            VMEM((4 * cut, width), BF16),
            VMEM((2, heads, width), BF16),
            VMEM(memory_state.shape, F32),
            VMEM((size, width), BF16),
            VMEM((2, width, inner), BF16),
            VMEM((inner, width), BF16),
            VMEM((n, rows, width), BF16),
            VMEM((n, rows, width), BF16),
            VMEM((n, rows, 128), F32),
            VMEM((n, rows, 4 * cut), BF16),
            VMEM((n, rows, 4 * cut), BF16),
            VMEM((n, 2 * hidden, shared_gate.shape[0]), BF16),
            VMEM((n, 2 * hidden, shared_gate.shape[0]), BF16),
            VMEM((n, hidden, shared_down.shape[1]), BF16),
            VMEM((heads, rows, size), BF16),
            VMEM((n, rows, size), BF16),
            VMEM((n, rows, width), F32),
            VMEM((2, chips, rows, width), BF16),
            VMEM((2, chips, rows, width), BF16),
            VMEM((2, chips, rows, width), BF16),
            VMEM((2, chips, rows, width), BF16),
            dma((10,)),
            dma((heads,)),
            dma((heads,)),
            dma((5, n)),
            dma((5, n)),
            dma((2, 4, chips)),
            dma((2, 2, chips)),
            dma((2, 2, chips)),
        ],
        compiler_params=pltpu.CompilerParams(
            collective_id=0, has_side_effects=True, vmem_limit_bytes=60 * 1024 * 1024
        ),
    )(*operands)


def fits(n, width, size, cut, hidden_all, experts, rows):
    return (
        n % 2 == 0
        and n <= 128
        and experts == n
        and width % (128 * n) == 0
        and hidden_all % (16 * n) == 0
        and size == 128
        and size % cut == 0
        and cut % 16 == 0
        and rows == 8
    )


def pick(n, *args):
    tokens, query_weight, memory_state = args[0], args[2], args[10]
    experts, hidden_all = args[18].shape[0] * n, args[21].shape[1]
    if fits(
        n, tokens.shape[1], memory_state.shape[3], query_weight.shape[1], hidden_all, experts,
        tokens.shape[0],
    ):
        return fused_shards(n, *args)
    return shards(*args)


def solution(mesh):
    placed = (
        P(("grp", "ep"), None),
        P(),
        P(None, "ep"),
        P(None, "ep"),
        P(None, "ep"),
        P(None, "ep"),
        P(),
        P(),
        P(),
        P(),
        P(("grp", "ep"), None, None, None),
        P(("grp", "ep"), None, None),
        P(("grp", "ep"), None),
        P(),
        P("ep", None),
        P(),
        P(("grp", "ep"), None),
        P(("grp", "ep"), None),
        P("ep", None, None),
        P("ep", None, None),
        P("ep", None, None),
        P("ep", None),
        P("ep", None),
        P(None, "ep"),
    )
    return jax.shard_map(
        functools.partial(pick, mesh.shape["ep"]),
        mesh=mesh,
        in_specs=placed,
        out_specs=(
            P(("grp", "ep"), None),
            P(("grp", "ep"), None, None, None),
            P(("grp", "ep"), None, None),
            P(("grp", "ep"), None),
        ),
        check_vma=False,
    )
```

```python
import jax
import jax.numpy as jnp
from jax import lax
from jax.experimental import pallas as pl
from jax.experimental.pallas import tpu as pltpu
from jax.sharding import PartitionSpec as P
import functools

epsilon = 1e-06


def rms_scale(values, gain):
    return (
        values
        * lax.rsqrt(jnp.mean(values * values, axis=-1, keepdims=True) + epsilon)
        * gain.astype(jnp.float32)
    )


def cell_step(
    normed,
    query,
    key_proj,
    value_proj,
    outgate,
    igate_weight,
    fgate_weight,
    igate_bias,
    fgate_bias,
    memory_state,
    norm_state,
    max_state,
    head_gain,
):
    row_count, head_count = max_state.shape
    head_size = memory_state.shape[-1]
    input_gate = jnp.dot(normed, igate_weight, preferred_element_type=jnp.float32) + igate_bias
    forget_log = jax.nn.log_sigmoid(
        jnp.dot(normed, fgate_weight, preferred_element_type=jnp.float32) + fgate_bias
    )
    query_heads = query.astype(jnp.float32).reshape(row_count, head_count, head_size)
    key_heads = key_proj.astype(jnp.float32).reshape(
        row_count, head_count, head_size
    ) * head_size ** (-0.5)
    value_heads = value_proj.astype(jnp.float32).reshape(row_count, head_count, head_size)
    max_next = jnp.maximum(forget_log + max_state, input_gate)
    decay_rate = jnp.exp(forget_log + max_state - max_next)
    injected = jnp.exp(input_gate - max_next)
    memory_next = decay_rate[:, :, None, None] * memory_state + injected[:, :, None, None] * (
        key_heads[:, :, :, None] * value_heads[:, :, None, :]
    )
    norm_next = decay_rate[:, :, None] * norm_state + injected[:, :, None] * key_heads
    numerator = jnp.einsum(
        "shd,shde->she", query_heads, memory_next, precision=lax.Precision.HIGHEST
    )
    denominator = jnp.maximum(
        jnp.abs(jnp.sum(query_heads * norm_next, axis=-1)), jnp.exp(-max_next)
    )
    readout = numerator / denominator[:, :, None]
    readout = rms_scale(readout, head_gain.reshape(head_count, head_size))
    gated = readout.reshape(row_count, head_count * head_size) * jax.nn.sigmoid(
        outgate.astype(jnp.float32)
    )
    return (gated.astype(jnp.bfloat16), memory_next, norm_next, max_next)


def shards(
    tokens,
    first_gain,
    query_weight,
    key_weight,
    value_weight,
    outgate_weight,
    igate_weight,
    fgate_weight,
    igate_bias,
    fgate_bias,
    memory_state,
    norm_state,
    max_state,
    head_gain,
    out_weight,
    second_gain,
    expert_ids,
    route_weight,
    expert_gate,
    expert_up,
    expert_down,
    shared_gate,
    shared_up,
    shared_down,
):
    own_rows = tokens.shape[0]
    devices = lax.axis_size("ep")
    top_count = expert_ids.shape[1]
    capacity = max(2, 2 * own_rows * top_count // devices)
    inputs = tokens.astype(jnp.float32)
    normed = rms_scale(inputs, first_gain).astype(jnp.bfloat16)
    block_rows = lax.all_gather(normed, "ep", axis=0, tiled=True)
    columns = jnp.stack(
        [
            jnp.dot(block_rows, matrix, preferred_element_type=jnp.float32).astype(jnp.bfloat16)
            for matrix in (query_weight, key_weight, value_weight, outgate_weight)
        ]
    )
    projected = lax.all_to_all(columns, "ep", split_axis=1, concat_axis=2, tiled=True)
    gated, memory_next, norm_next, max_next = cell_step(
        normed,
        projected[0],
        projected[1],
        projected[2],
        projected[3],
        igate_weight,
        fgate_weight,
        igate_bias,
        fgate_bias,
        memory_state,
        norm_state,
        max_state,
        head_gain,
    )
    picked = gated
    mix_sums = jnp.dot(
        picked,
        lax.all_gather(out_weight, "ep", axis=0, tiled=True),
        preferred_element_type=jnp.float32,
    )
    stream = inputs + mix_sums.astype(jnp.bfloat16).astype(jnp.float32)
    normed_two = rms_scale(stream, second_gain).astype(jnp.bfloat16)
    block_rows = (
        lax.all_gather(shared_gate, "ep", axis=0, tiled=True),
        lax.all_gather(shared_up, "ep", axis=0, tiled=True),
    )
    picked = normed_two
    gate_shared = jnp.dot(picked, block_rows[0], preferred_element_type=jnp.float32)
    up_shared = jnp.dot(picked, block_rows[1], preferred_element_type=jnp.float32)
    hidden_shared = (jax.nn.silu(gate_shared) * up_shared).astype(jnp.bfloat16)
    shared_result = jnp.dot(
        hidden_shared,
        lax.all_gather(shared_down, "ep", axis=1, tiled=True),
        preferred_element_type=jnp.float32,
    )
    choose = (expert_ids[:, :, None] == jnp.arange(devices, dtype=jnp.int32)[None, None, :]).astype(
        jnp.int32
    )
    counted = jnp.sum(choose, axis=1)
    ranking = jnp.cumsum(counted, axis=0) - counted
    slot_index = jnp.sum(choose * ranking[:, None, :], axis=2)
    slot_ids = jnp.arange(capacity, dtype=jnp.int32)
    selector = counted.T[:, None, :] * (ranking.T[:, None, :] == slot_ids[None, :, None]).astype(
        jnp.int32
    )
    outgoing = jnp.einsum(
        "ecr,rd->ecd", selector.astype(jnp.bfloat16), normed_two, preferred_element_type=jnp.float32
    ).astype(jnp.bfloat16)
    arrived = lax.all_to_all(outgoing, "ep", split_axis=0, concat_axis=0, tiled=True)
    sources, slots, width = arrived.shape
    flat_rows = arrived.reshape(sources * slots, width)
    gate_sums = jnp.dot(flat_rows, expert_gate[0], preferred_element_type=jnp.float32)
    up_sums = jnp.dot(flat_rows, expert_up[0], preferred_element_type=jnp.float32)
    hidden = (jax.nn.silu(gate_sums) * up_sums).astype(jnp.bfloat16)
    result = jnp.dot(hidden, expert_down[0], preferred_element_type=jnp.float32).astype(
        jnp.bfloat16
    )
    results = lax.all_to_all(
        result.reshape(sources, slots, width), "ep", split_axis=0, concat_axis=0, tiled=True
    )
    flat_results = results.reshape(devices * capacity, results.shape[2])
    picked_results = flat_results[expert_ids * capacity + slot_index]
    routed = jnp.sum(route_weight[:, :, None] * picked_results.astype(jnp.float32), axis=1)
    mixed_out = (stream + routed + shared_result).astype(jnp.bfloat16)
    return (mixed_out, memory_next, norm_next, max_next)


ANY, VMEM = pl.ANY, pltpu.VMEM
F32, BF16 = jnp.float32, jnp.bfloat16


def remote(source, target, send, receive, device):
    return pltpu.make_async_remote_copy(
        src_ref=source,
        dst_ref=target,
        send_sem=send,
        recv_sem=receive,
        device_id={"ep": device},
        device_id_type=pl.DeviceIdType.MESH,
    )


def across(left, right):
    return lax.dot_general(left, right, (((1,), (1,)), ((), ())), preferred_element_type=F32)


def in_line(gain):
    held = gain[...].astype(F32)
    return jnp.concatenate([held[i : i + 1] for i in range(held.shape[0])], axis=1)


def fused(
    n,
    tokens,
    first_gain,
    query_weight,
    key_weight,
    value_weight,
    outgate_weight,
    igate_weight,
    fgate_weight,
    igate_bias,
    fgate_bias,
    memory_state,
    norm_state,
    max_state,
    head_gain,
    out_weight,
    second_gain,
    expert_ids,
    route_weight,
    expert_gate,
    expert_up,
    expert_down,
    shared_gate,
    shared_up,
    shared_down,
    mixed_out,
    memory_next,
    norm_next,
    max_next,
    proj,
    gates_in,
    memory,
    out_pad,
    wide,
    down,
    rows_one,
    rows_two,
    table,
    column_send,
    column_recv,
    shared_send,
    shared_recv,
    sdown_recv,
    gated_send,
    gated_recv,
    part,
    part_send,
    pair_recv,
    sum_send,
    sum_recv,
    local_sem,
    memory_in_sem,
    send_sem,
    recv_sem,
    gather_sem,
    pair_sem,
    sum_sem,
):
    rows, width = tokens.shape
    heads, size = memory_state.shape[1], memory_state.shape[3]
    cut = query_weight.shape[0]
    share = size // cut
    hidden = shared_gate.shape[1] // n
    top_count = expert_ids.shape[1]
    chips = n // 2
    me = lax.axis_index("ep")
    side, chip = me % 2, me // 2
    partner = me + 1 - 2 * side

    barrier = pltpu.get_barrier_semaphore()
    for k in range(1, n):
        pl.semaphore_signal(
            barrier,
            inc=1,
            device_id={"ep": (me + k) % n},
            device_id_type=pl.DeviceIdType.MESH,
        )

    loads = []

    def load(source, target):
        copy = pltpu.make_async_copy(source, target, local_sem.at[len(loads)])
        copy.start()
        loads.append(copy)
        return copy

    proj_loads = [
        load(matrix, proj.at[pl.ds(i * cut, cut)])
        for i, matrix in enumerate((query_weight, key_weight, value_weight, outgate_weight))
    ]
    gate_loads = [load(igate_weight, gates_in.at[0]), load(fgate_weight, gates_in.at[1])]
    memory_loads = []
    for h in range(heads):
        copy = pltpu.make_async_copy(
            memory_state.at[:, h], memory.at[:, h], memory_in_sem.at[h]
        )
        copy.start()
        memory_loads.append(copy)
    spot = pl.multiple_of((me % share) * cut, cut)
    out_load = load(out_weight, out_pad.at[pl.ds(spot, cut)])
    wide_loads = [load(expert_gate.at[0], wide.at[0]), load(expert_up.at[0], wide.at[1])]
    down_load = load(expert_down.at[0], down)

    inputs = tokens[...].astype(F32)
    rows_one[me] = rms_scale(inputs, in_line(first_gain)).astype(BF16)

    pl.semaphore_wait(barrier, n - 1)

    def gather(buffer, which):
        sends = []
        for k in range(chips - 1, 0, -1):
            there = 2 * ((chip + k) % chips) + side
            sends.append(
                remote(
                    buffer.at[me],
                    buffer.at[me],
                    gather_sem.at[which, 0, k],
                    gather_sem.at[which, 1, k],
                    there,
                )
            )
            sends[-1].start()
        near = remote(
            buffer.at[me],
            buffer.at[me],
            gather_sem.at[which, 2, 0],
            gather_sem.at[which, 3, 0],
            partner,
        )
        near.start()
        return sends, near

    def gather_end(buffer, which, sends, near):
        passed = [near]
        for k in ORDER(chips):
            slot = 2 * ((chip + chips - k) % chips) + side
            sends[chips - 1 - k].wait_recv()
            onward = remote(
                buffer.at[slot],
                buffer.at[slot],
                gather_sem.at[which, 2, k],
                gather_sem.at[which, 3, k],
                partner,
            )
            onward.start()
            passed.append(onward)
        for copy in passed:
            copy.wait_recv()
        return sends + passed

    unsent = []
    first = gather(rows_one, 0)

    for i in range(1, share):
        other = pl.multiple_of(((me + i) % share) * cut, cut)
        out_pad[pl.ds(other, cut), :] = jnp.zeros((cut, width), BF16)
    lanes = lax.broadcasted_iota(jnp.int32, (rows, 128), 1)
    routes = jnp.zeros((rows, 128), F32)
    for t in range(top_count):
        routes = routes + jnp.where(
            expert_ids[:, t : t + 1] == lanes, route_weight[:, t : t + 1], 0.0
        )
    table[me] = routes
    for i, matrix in enumerate((shared_gate, shared_up)):
        turned = matrix[...].astype(F32).T.reshape(n, hidden, matrix.shape[0])
        shared_send[:, i * hidden : (i + 1) * hidden, :] = turned.astype(BF16)
    for copy in gate_loads:
        copy.wait()
    own = rows_one[me]
    input_gate = across(own, gates_in[0]) + igate_bias[...]
    forget_log = jax.nn.log_sigmoid(across(own, gates_in[1]) + fgate_bias[...])
    kept = forget_log + max_state[...]
    top = jnp.maximum(kept, input_gate)
    max_next[...] = top
    decay_rate = jnp.exp(kept - top)
    injected = jnp.exp(input_gate - top)
    floor = jnp.exp(-top)

    unsent += gather_end(rows_one, 0, *first)

    def flat(buffer):
        held = buffer[...].astype(F32)
        return held.reshape(n * rows, held.shape[2])

    for copy in proj_loads:
        copy.wait()
    columns = across(flat(rows_one).astype(BF16), proj[...])
    column_send[...] = columns.reshape(n, rows, 4 * cut).astype(BF16)

    def spread(which, source, target):
        for k in range(1, n):
            there = (me + k) % n
            copy = remote(
                source(there), target, send_sem.at[which, k], recv_sem.at[which, k], there
            )
            copy.start()
            unsent.append(copy)

    def arrive(which, source, target):
        for k in range(1, n):
            remote(
                source(me), target, send_sem.at[which, k], recv_sem.at[which, k], (me + k) % n
            ).wait_recv()

    spread(0, lambda j: column_send.at[j], column_recv.at[me])
    column_recv[me] = column_send[me]
    spread(1, lambda j: table.at[me], table.at[me])
    arrive(0, lambda j: column_send.at[j], column_recv.at[me])
    spread(2, lambda j: shared_send.at[j], shared_recv.at[me])
    shared_recv[me] = shared_send[me]
    spread(3, lambda j: shared_down.at[j], sdown_recv.at[me])
    sdown_recv[me] = shared_down[me]

    for h in range(heads):
        pieces = [column_recv[h * share + i].astype(F32) for i in range(share)]
        query, keyed, valued, outgate = [
            jnp.concatenate([piece[:, i * cut : (i + 1) * cut] for piece in pieces], axis=1)
            for i in range(4)
        ]
        decay = jnp.broadcast_to(decay_rate[:, h : h + 1], (rows, size))
        inject = keyed * size ** (-0.5) * injected[:, h : h + 1]
        norm = decay * norm_state[:, h, :] + inject
        norm_next[:, h, :] = norm
        bottom = jnp.maximum(
            jnp.abs(jnp.sum(query * norm, axis=-1, keepdims=True)), floor[:, h : h + 1]
        )
        key_columns, query_columns = inject.T, query.T
        memory_loads[h].wait()
        tops = []
        for s in range(rows):
            cell = (
                decay[s : s + 1, :] * memory[s, h]
                + key_columns[:, s : s + 1] * valued[s : s + 1, :]
            )
            memory_next[s, h] = cell
            tops.append(jnp.sum(query_columns[:, s : s + 1] * cell, axis=0, keepdims=True))
        readout = jnp.concatenate(tops, axis=0) / bottom
        readout = rms_scale(readout, head_gain[h : h + 1, :])
        gated_send[h] = (readout * jax.nn.sigmoid(outgate)).astype(BF16)

    spread(4, lambda j: gated_send.at[j // share], gated_recv.at[me])
    gated_recv[me] = gated_send[me // share]
    out_load.wait()
    arrive(4, lambda j: gated_send.at[j // share], gated_recv.at[me])

    def scatter(which, total, value):
        part[...] = value.reshape(n, rows, width)
        pair = []
        for k in list(range(1, chips)) + [0]:
            c = (chip + k) % chips
            part_send[which, c] = part[2 * c + 1 - side].astype(BF16)
            copy = remote(
                part_send.at[which, c],
                pair_recv.at[which, c],
                pair_sem.at[which, 0, k],
                pair_sem.at[which, 1, k],
                partner,
            )
            copy.start()
            pair.append((k, c, copy))
        sends = []
        for k, c, copy in pair:
            copy.wait_recv()
            both = part[2 * c + side] + pair_recv[which, c].astype(F32)
            if k == 0:
                total = total + both if total is not None else both
                continue
            sum_send[which, c] = both.astype(BF16)
            away = remote(
                sum_send.at[which, c],
                sum_recv.at[which, chip],
                sum_sem.at[which, 0, k],
                sum_sem.at[which, 1, k],
                2 * c + side,
            )
            away.start()
            sends.append((k, away))
        for k, away in sends:
            away.wait_recv()
            total = total + sum_recv[which, (chip + chips - k) % chips].astype(F32)
        unsent.extend([copy for _, _, copy in pair] + [away for _, away in sends])
        return total

    mix = scatter(
        0, None, jnp.dot(flat(gated_recv).astype(BF16), out_pad[...], preferred_element_type=F32)
    )
    stream = tokens[...].astype(F32) + mix.astype(BF16).astype(F32)
    rows_two[me] = rms_scale(stream, in_line(second_gain)).astype(BF16)
    second = gather(rows_two, 1)
    for copy in wide_loads + [down_load]:
        copy.wait()
    arrive(1, lambda j: table.at[me], table.at[me])
    arrive(2, lambda j: shared_send.at[j], shared_recv.at[me])
    arrive(3, lambda j: shared_down.at[j], sdown_recv.at[me])
    weights = flat(table)
    mine = lax.broadcasted_iota(jnp.int32, weights.shape, 1) == me
    weight = jnp.sum(jnp.where(mine, weights, 0.0), axis=1, keepdims=True)
    shared_wide = jnp.concatenate([shared_recv[i] for i in range(n)], axis=1)
    shared_rows = jnp.concatenate([sdown_recv[i] for i in range(n)], axis=1)
    unsent += gather_end(rows_two, 1, *second)

    block = flat(rows_two).astype(BF16)
    gate_sums = jnp.dot(block, wide[0], preferred_element_type=F32)
    up_sums = jnp.dot(block, wide[1], preferred_element_type=F32)
    own_hidden = (jax.nn.silu(gate_sums) * up_sums).astype(BF16)
    both = across(block, shared_wide)
    shared_hidden = (jax.nn.silu(both[:, :hidden]) * both[:, hidden:]).astype(BF16)
    value = weight * jnp.dot(own_hidden, down[...], preferred_element_type=F32) + jnp.dot(
        shared_hidden, shared_rows, preferred_element_type=F32
    )
    mixed_out[...] = scatter(1, stream, value).astype(BF16)

    for copy in unsent:
        copy.wait_send()


def ORDER(chips):
    return range(chips - 1, 0, -1)


def fused_shards(n, *args):
    (tokens, first_gain, query_weight, key_weight, value_weight, outgate_weight, igate_weight,
     fgate_weight, igate_bias, fgate_bias, memory_state, norm_state, max_state, head_gain,
     out_weight, second_gain, expert_ids, route_weight, expert_gate, expert_up, expert_down,
     shared_gate, shared_up, shared_down) = args
    rows, width = tokens.shape
    heads, size = memory_state.shape[1], memory_state.shape[3]
    cut = query_weight.shape[1]
    hidden = shared_gate.shape[1] // n
    chips = n // 2
    inner = expert_gate.shape[2]
    operands = (
        tokens, first_gain.reshape(-1, 128), query_weight.T, key_weight.T, value_weight.T,
        outgate_weight.T, igate_weight.T, fgate_weight.T, igate_bias.reshape(1, -1), fgate_bias.reshape(1, -1),
        memory_state, norm_state, max_state, head_gain.reshape(heads, size), out_weight,
        second_gain.reshape(-1, 128), expert_ids, route_weight, expert_gate, expert_up, expert_down,
        shared_gate, shared_up, shared_down.reshape(n, hidden, shared_down.shape[1]),
    )
    far = {2, 3, 4, 5, 6, 7, 10, 14, 18, 19, 20}
    operands = [
        pltpu.with_memory_space_constraint(x, pltpu.HBM)
        for i, x in enumerate(operands)
    ]
    dma = pltpu.SemaphoreType.DMA
    return pl.pallas_call(
        functools.partial(fused, n),
        out_shape=(
            jax.ShapeDtypeStruct((rows, width), BF16),
            jax.ShapeDtypeStruct(memory_state.shape, F32),
            jax.ShapeDtypeStruct(norm_state.shape, F32),
            jax.ShapeDtypeStruct(max_state.shape, F32),
        ),
        in_specs=[
            pl.BlockSpec(memory_space=pltpu.HBM if i in far else VMEM) for i in range(len(operands))
        ],
        out_specs=tuple(pl.BlockSpec(memory_space=m) for m in (VMEM, VMEM, VMEM, VMEM)),
        scratch_shapes=[
            VMEM((4 * cut, width), BF16),
            VMEM((2, heads, width), BF16),
            VMEM(memory_state.shape, F32),
            VMEM((size, width), BF16),
            VMEM((2, width, inner), BF16),
            VMEM((inner, width), BF16),
            VMEM((n, rows, width), BF16),
            VMEM((n, rows, width), BF16),
            VMEM((n, rows, 128), F32),
            VMEM((n, rows, 4 * cut), BF16),
            VMEM((n, rows, 4 * cut), BF16),
            VMEM((n, 2 * hidden, shared_gate.shape[0]), BF16),
            VMEM((n, 2 * hidden, shared_gate.shape[0]), BF16),
            VMEM((n, hidden, shared_down.shape[1]), BF16),
            VMEM((heads, rows, size), BF16),
            VMEM((n, rows, size), BF16),
            VMEM((n, rows, width), F32),
            VMEM((2, chips, rows, width), BF16),
            VMEM((2, chips, rows, width), BF16),
            VMEM((2, chips, rows, width), BF16),
            VMEM((2, chips, rows, width), BF16),
            dma((10,)),
            dma((heads,)),
            dma((5, n)),
            dma((5, n)),
            dma((2, 4, chips)),
            dma((2, 2, chips)),
            dma((2, 2, chips)),
        ],
        compiler_params=pltpu.CompilerParams(
            collective_id=0, has_side_effects=True, vmem_limit_bytes=28 * 1024 * 1024
        ),
    )(*operands)


def fits(n, width, size, cut, hidden_all, experts, rows):
    return (
        n % 2 == 0
        and n <= 128
        and experts == n
        and width % (128 * n) == 0
        and hidden_all % (16 * n) == 0
        and size == 128
        and size % cut == 0
        and cut % 16 == 0
        and rows == 8
    )


def pick(n, *args):
    tokens, query_weight, memory_state = args[0], args[2], args[10]
    experts, hidden_all = args[18].shape[0] * n, args[21].shape[1]
    if fits(
        n, tokens.shape[1], memory_state.shape[3], query_weight.shape[1], hidden_all, experts,
        tokens.shape[0],
    ):
        return fused_shards(n, *args)
    return shards(*args)


def solution(mesh):
    placed = (
        P(("grp", "ep"), None),
        P(),
        P(None, "ep"),
        P(None, "ep"),
        P(None, "ep"),
        P(None, "ep"),
        P(),
        P(),
        P(),
        P(),
        P(("grp", "ep"), None, None, None),
        P(("grp", "ep"), None, None),
        P(("grp", "ep"), None),
        P(),
        P("ep", None),
        P(),
        P(("grp", "ep"), None),
        P(("grp", "ep"), None),
        P("ep", None, None),
        P("ep", None, None),
        P("ep", None, None),
        P("ep", None),
        P("ep", None),
        P(None, "ep"),
    )
    return jax.shard_map(
        functools.partial(pick, mesh.shape["ep"]),
        mesh=mesh,
        in_specs=placed,
        out_specs=(
            P(("grp", "ep"), None),
            P(("grp", "ep"), None, None, None),
            P(("grp", "ep"), None, None),
            P(("grp", "ep"), None),
        ),
        check_vma=False,
    )
```
